32 devices in a mesh: sp: 16 (over z, y, x), tp: 2 (over core).
Axes of the slice: x: 2, y: 2, z: 4, core: 2. Of those that a mesh axis runs over, the one named last changes fastest.
Arguments:
- activations: bfloat16 [2048, 2048], P('sp', 'tp'), may hold values from -200 to 200
- norm_gain: float32 [2048], replicated, may hold values from 0.1 to 1.9
- state_proj: bfloat16 [2048, 1024], P(None, 'tp'), may hold values from -0.125 to 0.125
- value_proj: bfloat16 [2048, 1024], P(None, 'tp'), may hold values from -0.125 to 0.125
- post_gate_proj: bfloat16 [2048, 1024], P(None, 'tp'), may hold values from -0.125 to 0.125
- pre_gate_proj: bfloat16 [2048, 1024], P(None, 'tp'), may hold values from -0.125 to 0.125
- input_map: bfloat16 [64, 16, 128], P('tp'), may hold values from -1.5 to 1.5
- output_map: float32 [64, 128, 16], P('tp'), may hold values from -0.5 to 0.5
- skip_gain: float32 [1024], P('tp'), may hold values from -4 to 4
- rotation: float32 [64, 64], P('tp'), may hold values from -3.140625 to 3.140625
- log_decay: float32 [2048, 64], P('sp', 'tp'), may hold values from -1.5 to 0, as said below
- initial_state: float32 [2, 64, 64], P(None, 'tp'), may hold values from -12 to 12
- conv_taps: bfloat16 [3, 1024], P(None, 'tp'), may hold values from -3.5 to 3.5
- state_out: bfloat16 [1024, 2048], P(None, 'tp'), may hold values from -0.125 to 0.125
- conv_out: bfloat16 [1024, 2048], P(None, 'tp'), may hold values from -0.125 to 0.125
Outputs:
- layer_out: bfloat16 [2048, 2048], P('sp', 'tp')
The draws below stay inside these ranges and needn't reach their ends.
Inputs may be any that keep to these rules, and one draw needn't show every extreme that they name: `log_decay`: every entry is negative.
All inputs are finite; a program needn't handle non-finite values.
Results may differ from the reference program's by a relative error of at most 0.014.
Values may be sent and summed in bfloat16 or wider, within the bound.
A program may use at most 64 MiB of HBM per device.

```python
import math
import jax
import jax.numpy as jnp
from jax import lax

D = 2048
GROUP_CH = 16
STATE = 64
CONV_W = 3
TOK_DEV = 128
D_SSM = 1024
D_CONV = 1024
GROUPS = 64
TOKENS = 2048


def draw_activations(key, part):
    key_base, key_rows = jax.random.split(key, 2)
    column = jnp.arange(D, dtype=jnp.float32) / (D - 1)
    base = jnp.clip(jax.random.normal(key_base, (TOKENS, D), jnp.float32), -5.0, 5.0)
    row_scale = jnp.exp(jax.random.uniform(key_rows, (TOKENS, 1), jnp.float32, 0.0, math.log(4.0)))
    col_scale = jnp.exp(column * math.log(4.0))
    return (base * row_scale * col_scale[None, :]).astype(jnp.bfloat16)


def draw_log_decay(key, part):
    keys = jax.random.split(key, 5)
    share = 0.5
    slow = jax.random.bernoulli(keys[0], share, (1, GROUPS))
    blocks = TOKENS // TOK_DEV
    factor = jnp.exp(jax.random.uniform(keys[1], (blocks, 1, GROUPS), jnp.float32, 0.0, math.log(3.0)))
    factor = jnp.broadcast_to(factor, (blocks, TOK_DEV, GROUPS)).reshape(TOKENS, GROUPS)
    rough = jax.random.uniform(keys[2], (TOKENS, GROUPS), jnp.float32, 0.5, 1.5)
    rate = jnp.where(slow, 0.35 / TOKENS, 0.02)
    value = -rate * factor * rough
    spots = jax.random.randint(keys[3], (2, GROUPS), 0, TOKENS)
    depth = jnp.log(jax.random.uniform(keys[4], (2, GROUPS), jnp.float32, 0.5, 0.8))
    hit = jnp.arange(TOKENS, dtype=jnp.int32)[:, None, None] == spots[None, :, :]
    value = value + jnp.sum(jnp.where(hit, depth[None, :, :], 0.0), axis=1)
    return value.astype(jnp.float32)


def block_scale(key, dims, cuts, low, largest):
    def one(dim, blocks):
        steps = jax.random.uniform(jax.random.fold_in(jax.random.fold_in(key, 6), dim), (blocks,), jnp.float32, low / len(cuts), largest / len(cuts))
        return jnp.repeat(jnp.exp(steps), dims[dim] // blocks).reshape((-1,) + (1,) * (len(dims) - dim - 1))

    gain = one(*cuts[0])
    for cut in cuts[1:]:
        gain = gain * one(*cut)
    return gain


def gaussian(own_key, dims, width, reach, pieces=(), kind=jnp.bfloat16):
    values = jax.random.normal(own_key, dims, jnp.float32) * width
    if len(pieces) > 0:
        values = block_scale(own_key, dims, pieces, -0.22, 0.18) * values
    return jnp.clip(values, min=-reach, max=reach).astype(kind)


def setup_inputs(seed: int = 0) -> dict:
    arg_keys = jax.random.split(jax.random.key(seed), 16)
    activations = draw_activations(jax.random.fold_in(arg_keys[15], 71), 0)
    norm_gain = jnp.clip(1.0 + 0.18 * jax.random.normal(arg_keys[1], (D,), jnp.float32), 0.1, 1.9)
    state_proj = gaussian(arg_keys[2], (D, D_SSM), D ** -0.5, 0.125, ((1, 2),))
    value_proj = gaussian(arg_keys[3], (D, D_CONV), D ** -0.5, 0.125, ((1, 2),))
    post_gate_proj = gaussian(arg_keys[4], (D, D_CONV), D ** -0.5, 0.125, ((1, 2),))
    pre_gate_proj = gaussian(arg_keys[5], (D, D_CONV), D ** -0.5, 0.125, ((1, 2),))
    input_map = gaussian(arg_keys[6], (GROUPS, GROUP_CH, 2 * STATE), GROUP_CH ** -0.5, 1.5, ((0, 2),))
    output_map = gaussian(arg_keys[7], (GROUPS, 2 * STATE, GROUP_CH), (2 * STATE) ** -0.5, 0.5, ((0, 2),), jnp.float32)
    skip_gain = gaussian(arg_keys[8], (D_SSM,), 1.0, 4.0, ((0, 2),), jnp.float32)
    rotation = jnp.clip(jax.random.uniform(arg_keys[9], (GROUPS, STATE), jnp.float32, -3.140625, 3.140625), -3.140625, 3.140625)
    log_decay = draw_log_decay(jax.random.fold_in(arg_keys[15], 71), 0)
    initial_state = gaussian(arg_keys[11], (2, GROUPS, STATE), 2.0, 12.0, ((1, 2),), jnp.float32)
    conv_taps = gaussian(arg_keys[12], (CONV_W, D_CONV), CONV_W ** -0.5, 3.5, ((1, 2),))
    state_out = gaussian(arg_keys[13], (D_SSM, D), (D_SSM + D_CONV) ** -0.5, 0.125, ((1, 2),))
    conv_out = gaussian(arg_keys[14], (D_CONV, D), (D_SSM + D_CONV) ** -0.5, 0.125, ((1, 2),))
    return dict(activations=activations, norm_gain=norm_gain, state_proj=state_proj, value_proj=value_proj, post_gate_proj=post_gate_proj, pre_gate_proj=pre_gate_proj, input_map=input_map, output_map=output_map, skip_gain=skip_gain, rotation=rotation, log_decay=log_decay, initial_state=initial_state, conv_taps=conv_taps, state_out=state_out, conv_out=conv_out)


EPS = 1e-06

def combine(earlier, later):
    early_are, early_aim, early_hre, early_him = earlier
    late_are, late_aim, late_hre, late_him = later
    return (early_are * late_are - early_aim * late_aim, early_are * late_aim + early_aim * late_are, late_are * early_hre - late_aim * early_him + late_hre, late_are * early_him + late_aim * early_hre + late_him)

def reference(activations, norm_gain, state_proj, value_proj, post_gate_proj, pre_gate_proj, input_map, output_map, skip_gain, rotation, log_decay, initial_state, conv_taps, state_out, conv_out):
    span = math.gcd(TOKENS, 512)
    count = TOKENS // span
    states = GROUPS * STATE
    cos_rot = jnp.cos(rotation).reshape(1, states)
    sin_rot = jnp.sin(rotation).reshape(1, states)
    weights_in = (state_proj, value_proj, post_gate_proj, pre_gate_proj)
    taps = conv_taps.astype(jnp.float32)

    def block_step(carry, index):
        h_re, h_im, tail = carry
        start = (index * span).astype(jnp.int32)
        rows = lax.dynamic_slice_in_dim(activations, start, span, 0)
        decay = lax.dynamic_slice_in_dim(log_decay, start, span, 0)
        wide = rows.astype(jnp.float32)
        scale = lax.rsqrt(lax.optimization_barrier(jnp.mean(wide * wide, axis=1, keepdims=True)) + EPS)
        scaled = (wide * norm_gain[None, :]).astype(jnp.bfloat16)
        drive_in, value, post_gate, pre_gate = [(jnp.dot(scaled, weight, preferred_element_type=jnp.float32) * scale).astype(jnp.bfloat16) for weight in weights_in]
        grouped = drive_in.reshape(span, GROUPS, GROUP_CH).astype(jnp.float32)
        drive = jnp.einsum('tgc,gck->tgk', grouped, input_map.astype(jnp.float32))
        drive = drive * jnp.sqrt(-jnp.expm1(2.0 * decay))[:, :, None]
        drive_re = drive[:, :, :STATE].reshape(span, states)
        drive_im = drive[:, :, STATE:].reshape(span, states)
        magnitude = jnp.repeat(jnp.exp(decay), STATE, axis=1)
        factor_re = magnitude * cos_rot
        factor_im = magnitude * sin_rot
        cum_re, cum_im, loc_re, loc_im = lax.associative_scan(combine, (factor_re, factor_im, drive_re, drive_im), axis=0)
        state_re = loc_re + cum_re * h_re - cum_im * h_im
        state_im = loc_im + cum_re * h_im + cum_im * h_re
        stacked = jnp.concatenate([state_re.reshape(span, GROUPS, STATE), state_im.reshape(span, GROUPS, STATE)], axis=2)
        read = jnp.einsum('tgk,gkc->tgc', stacked, output_map, precision=lax.Precision.HIGHEST).reshape(span, D_SSM)
        hidden_state = jax.nn.gelu(read + skip_gain[None, :] * drive_in.astype(jnp.float32)).astype(jnp.bfloat16)
        mixed_in = (pre_gate.astype(jnp.float32) * value.astype(jnp.float32)).astype(jnp.bfloat16)
        padded = jnp.concatenate([tail, mixed_in], axis=0)
        conv = jnp.zeros((span, D_CONV), jnp.float32)
        for k in range(CONV_W):
            conv = conv + padded[k:k + span].astype(jnp.float32) * taps[k][None, :]
        hidden_conv = (post_gate.astype(jnp.float32) * conv).astype(jnp.bfloat16)
        result = (jnp.dot(hidden_state, state_out, preferred_element_type=jnp.float32) + jnp.dot(hidden_conv, conv_out, preferred_element_type=jnp.float32)).astype(jnp.bfloat16)
        return ((state_re[span - 1:], state_im[span - 1:], padded[span:]), result)
    start_carry = (initial_state[0].reshape(1, states).astype(jnp.float32), initial_state[1].reshape(1, states).astype(jnp.float32), jnp.zeros((CONV_W - 1, D_CONV), jnp.bfloat16))
    ignored, blocks = lax.scan(block_step, start_carry, jnp.arange(count, dtype=jnp.int32))
    return blocks.reshape(TOKENS, D)
```

```python
import functools

import jax
import jax.numpy as jnp
from jax import lax
from jax.experimental import pallas as pl
from jax.experimental.pallas import tpu as pltpu
from jax.sharding import PartitionSpec as P

EPS = 1e-06
LANES = 128
MESH = pl.DeviceIdType.MESH
F32 = jnp.float32
BF16 = jnp.bfloat16


def minus_expm1(y):
    poly = jnp.ones_like(y)
    for k in range(11, 1, -1):
        poly = 1.0 + poly * y * (1.0 / k)
    return jnp.where(y > -0.5, -y * poly, 1.0 - jnp.exp(y))


def split3(v):
    hi = v.astype(BF16)
    rest = v - hi.astype(F32)
    mid = rest.astype(BF16)
    low = (rest - mid.astype(F32)).astype(BF16)
    return hi, mid, low


def cmul(a, b):
    return a[0] * b[0] - a[1] * b[1], a[0] * b[1] + a[1] * b[0]


def cpow(base, count):
    result = None
    while count:
        if count & 1:
            result = base if result is None else cmul(result, base)
        count >>= 1
        if count:
            base = cmul(base, base)
    return result


def gelu(x):
    return 0.5 * x * (1.0 + jnp.tanh(0.7978845608028654 * (x + 0.044715 * x * x * x)))


def kernel(
    n,
    x_ref,
    gain_ref,
    w0_hbm,
    w1_hbm,
    w2_hbm,
    w3_hbm,
    imap_ref,
    omap_ref,
    skip_ref,
    rot_ref,
    ld_ref,
    init_ref,
    taps_ref,
    so_hbm,
    co_hbm,
    out_ref,
    wv,
    ov,
    xr,
    acc,
    din,
    bd_in,
    bd_out,
    wide_w,
    mag,
    drv,
    pairs,
    pad,
    pay,
    ends,
    hs,
    hc,
    oacc,
    wsem,
    osem,
    x_sem,
    tail_sem,
    hc_sem,
    hs_sem,
    send_sem,
    recv_sem,
):
    sp, tp = lax.axis_index("sp"), lax.axis_index("tp")
    other = 1 - tp
    rows, half = x_ref.shape
    groups, state = rot_ref.shape
    gch = imap_ref.shape[1]
    chans = groups * gch
    states = groups * state
    prow = states // LANES
    per_block = LANES // gch
    blocks = groups // per_block
    quads = prow // blocks
    bstates = quads * LANES
    cwide = taps_ref.shape[1]
    width = taps_ref.shape[0]

    barrier = pltpu.get_barrier_semaphore()

    def greet(j, c):
        pl.semaphore_signal(
            barrier, inc=1, device_id={"sp": lax.rem(sp + j, n), "tp": tp}, device_id_type=MESH
        )
        return c

    pl.semaphore_signal(barrier, inc=1, device_id={"sp": sp, "tp": other}, device_id_type=MESH)
    lax.fori_loop(1, n, greet, 0)

    wcopies = {}
    for h, part in ((0, tp), (1, other)):
        for i, w in enumerate((w0_hbm, w1_hbm, w2_hbm, w3_hbm)):
            copy = pltpu.make_async_copy(
                w.at[pl.ds(part * half, half), :], wv.at[i, h], wsem.at[i, h]
            )
            copy.start()
            wcopies[i, h] = copy
    ocopies = {}
    for i, w, deep in ((1, co_hbm, cwide), (0, so_hbm, chans)):
        for h, part in ((0, tp), (1, other)):
            copy = pltpu.make_async_copy(w.at[pl.ds(part * deep, deep), :], ov.at[i, h], osem.at[i, h])
            copy.start()
            ocopies[i, h] = copy

    lane = lax.broadcasted_iota(jnp.int32, (1, LANES), 1)
    for i, v in enumerate((rot_ref[...], init_ref[0], init_ref[1])):
        pairs[pl.ds(i * groups, groups), :] = jnp.concatenate([v, v], axis=1)

    def paired(i):
        even = pairs[pl.ds(i * groups, prow, stride=2), :]
        odd = pairs[pl.ds(i * groups + 1, prow, stride=2), :]
        return jnp.where(lane < state, even, odd)

    theta = paired(0)
    cosv, sinv = jnp.cos(theta), jnp.sin(theta)
    whole = cpow((cosv, sinv), rows)

    for src, dst in ((imap_ref, bd_in), (omap_ref, bd_out)):
        dst[...] = jnp.zeros_like(dst)
        for b in range(blocks):
            for q in range(quads):
                g = b * per_block + 2 * q
                one = src[g].astype(F32)
                two = src[g + 1].astype(F32)
                one_r = jnp.concatenate([one[:, state:], one[:, :state]], axis=1)
                two_r = jnp.concatenate([two[:, state:], two[:, :state]], axis=1)
                low = lane < state
                re = jnp.concatenate([jnp.where(low, one, 0.0), jnp.where(low, 0.0, two_r)], axis=0)
                im = jnp.concatenate([jnp.where(low, one_r, 0.0), jnp.where(low, 0.0, two)], axis=0)
                at = pl.ds(b * LANES + q * 2 * gch, 2 * gch)
                dst[at, q * LANES : (q + 1) * LANES] = re.astype(BF16)
                dst[at, bstates + q * LANES : bstates + (q + 1) * LANES] = im.astype(BF16)

    ld = ld_ref[...].T
    mags = split3(jnp.exp(ld))
    gains = split3(jnp.sqrt(minus_expm1(2.0 * ld)))[:2]
    for b in range(blocks):
        col = lax.broadcasted_iota(jnp.int32, (groups, bstates), 1) + b * bstates
        row = lax.broadcasted_iota(jnp.int32, (groups, bstates), 0)
        spread = jnp.where(
            (col >= row * state) & (col < (row + 1) * state), 1.0, 0.0
        ).astype(BF16)

        def over(pieces):
            total = None
            for piece in pieces:
                d = jnp.dot(piece, spread, preferred_element_type=F32)
                total = d if total is None else total + d
            return total

        m = over(mags)
        for q in range(quads):
            mag[pl.ds(b * quads + q, rows, stride=prow), :] = m[:, q * LANES : (q + 1) * LANES]
        wide_w[:, b * bstates : (b + 1) * bstates] = over(gains)

    pl.semaphore_wait(barrier, n)
    partner = {"sp": sp, "tp": other}

    def remote(src, dst, s, r, dev):
        return pltpu.make_async_remote_copy(
            src_ref=src, dst_ref=dst, send_sem=s, recv_sem=r, device_id=dev, device_id_type=MESH
        )

    x_copy = remote(x_ref, xr, x_sem.at[0], x_sem.at[1], partner)
    x_copy.start()

    own = x_ref[...].astype(F32)
    scaled = (own * gain_ref[:, pl.ds(pl.multiple_of(tp * half, LANES), half)]).astype(BF16)
    squares = jnp.sum(own * own, axis=1, keepdims=True)
    for i in range(4):
        wcopies[i, 0].wait()
        acc[i] = jnp.dot(scaled, wv[i, 0], preferred_element_type=F32)

    x_copy.wait_recv()
    far = xr[...].astype(F32)
    scaled_far = (far * gain_ref[:, pl.ds(pl.multiple_of(other * half, LANES), half)]).astype(BF16)
    squares = squares + jnp.sum(far * far, axis=1, keepdims=True)
    scale = lax.rsqrt(squares / (2 * half) + EPS)

    def project(i):
        wcopies[i, 1].wait()
        total = acc[i] + jnp.dot(scaled_far, wv[i, 1], preferred_element_type=F32)
        return (total * scale).astype(BF16)

    drive_in = project(0)
    din[...] = drive_in
    for b in range(blocks):
        blk = jnp.dot(
            drive_in[:, b * LANES : (b + 1) * LANES],
            bd_in[b * LANES : (b + 1) * LANES, :],
            preferred_element_type=F32,
        )
        for q in range(quads):
            r = b * quads + q
            w = wide_w[:, r * LANES : (r + 1) * LANES]
            drv[pl.ds(r, rows, stride=2 * prow), :] = blk[:, q * LANES : (q + 1) * LANES] * w
            drv[pl.ds(prow + r, rows, stride=2 * prow), :] = (
                blk[:, bstates + q * LANES : bstates + (q + 1) * LANES] * w
            )

    def advance(t, h):
        m = mag[pl.ds(pl.multiple_of(t * prow, prow), prow), :]
        base = pl.multiple_of(t * 2 * prow, 2 * prow)
        d_re = drv[pl.ds(base, prow), :]
        d_im = drv[pl.ds(base + prow, prow), :]
        f_re, f_im = m * cosv, m * sinv
        new_re = (f_re * h[0] + d_re) - f_im * h[1]
        new_im = (f_re * h[1] + d_im) + f_im * h[0]
        return m, base, (new_re, new_im)

    def first(t, c):
        m, base, h = advance(t, c[:2])
        return h[0], h[1], c[2] * m

    zero = jnp.zeros((prow, LANES), F32)
    e_re, e_im, e_mag = lax.fori_loop(0, rows, first, (zero, zero, zero + 1.0), unroll=8)
    pay[pl.ds(0, prow), :] = e_re
    pay[pl.ds(prow, prow), :] = e_im
    pay[pl.ds(2 * prow, prow), :] = e_mag

    def end_copy(j):
        return remote(
            pay, ends.at[sp], send_sem.at[j], recv_sem.at[sp], {"sp": j, "tp": tp}
        )

    def send_end(j, c):
        end_copy(j).start()
        return c

    lax.fori_loop(sp + 1, n, send_end, 0)

    value = project(1)
    pre_gate = project(3)
    mixed = (pre_gate.astype(F32) * value.astype(F32)).astype(BF16).astype(F32)
    pad[pl.ds(8, rows), :] = mixed
    tail_copy = remote(
        pad.at[pl.ds(rows, 8), :],
        pad.at[pl.ds(0, 8), :],
        tail_sem.at[0],
        tail_sem.at[1],
        {"sp": lax.rem(sp + 1, n), "tp": tp},
    )

    @pl.when(sp < n - 1)
    def _():
        tail_copy.start()

    post_gate = project(2).astype(F32)

    @pl.when(sp == 0)
    def _():
        pad[pl.ds(0, 8), :] = jnp.zeros((8, cwide), F32)

    @pl.when(sp > 0)
    def _():
        tail_copy.wait_recv()

    conv = jnp.zeros((rows, cwide), F32)
    for k in range(width):
        conv = conv + pad[pl.ds(8 + k - (width - 1), rows), :] * taps_ref[k : k + 1, :].astype(F32)
    hc[0] = (post_gate * conv).astype(BF16)
    hc_copy = remote(hc.at[0], hc.at[1], hc_sem.at[0], hc_sem.at[1], partner)
    hc_copy.start()
    ocopies[1, 0].wait()
    ocopies[1, 1].wait()
    oacc[...] = jnp.dot(hc[0], ov[1, 0], preferred_element_type=F32)
    hc_copy.wait_recv()
    oacc[...] += jnp.dot(hc[1], ov[1, 1], preferred_element_type=F32)

    def gather(k, h):
        remote(pay, ends.at[k], send_sem.at[k], recv_sem.at[k], {"sp": k, "tp": tp}).wait_recv()
        k_mag = ends[k, pl.ds(2 * prow, prow), :]
        moved = cmul((whole[0] * k_mag, whole[1] * k_mag), h)
        return moved[0] + ends[k, pl.ds(0, prow), :], moved[1] + ends[k, pl.ds(prow, prow), :]

    enter = lax.fori_loop(0, sp, gather, (paired(1), paired(2)))

    def second(t, c):
        m, base, h = advance(t, c)
        drv[pl.ds(base, prow), :] = h[0]
        drv[pl.ds(base + prow, prow), :] = h[1]
        return h

    lax.fori_loop(0, rows, second, enter, unroll=8)

    hs_copies = []
    for b in range(blocks):
        at = [b * quads + q for q in range(quads)]
        at = at + [prow + r for r in at]
        cols = slice(b * LANES, (b + 1) * LANES)
        st = jnp.concatenate(
            [drv[pl.ds(r, rows, stride=2 * prow), :].astype(BF16) for r in at], axis=1
        )
        read = lax.dot_general(
            st, bd_out[cols, :], (((1,), (1,)), ((), ())), preferred_element_type=F32
        )
        hs[0, :, cols] = gelu(read + skip_ref[:, cols] * din[:, cols].astype(F32)).astype(BF16)
        if b % 2 == 1:
            two = pl.ds((b - 1) * LANES, 2 * LANES)
            copy = remote(
                hs.at[0, :, two], hs.at[1, :, two], hs_sem.at[0, b // 2], hs_sem.at[1, b // 2], partner
            )
            copy.start()
            hs_copies.append(copy)
    ocopies[0, 0].wait()
    ocopies[0, 1].wait()
    oacc[...] += jnp.dot(hs[0], ov[0, 0], preferred_element_type=F32)
    for copy in hs_copies:
        copy.wait_recv()
    out_ref[...] = (oacc[...] + jnp.dot(hs[1], ov[0, 1], preferred_element_type=F32)).astype(BF16)

    x_copy.wait_send()
    hc_copy.wait_send()
    for copy in hs_copies:
        copy.wait_send()

    @pl.when(sp < n - 1)
    def _():
        tail_copy.wait_send()

    def sent(j, c):
        end_copy(j).wait_send()
        return c

    lax.fori_loop(sp + 1, n, sent, 0)


def on_device(
    activations,
    norm_gain,
    state_proj,
    value_proj,
    post_gate_proj,
    pre_gate_proj,
    input_map,
    output_map,
    skip_gain,
    rotation,
    log_decay,
    initial_state,
    conv_taps,
    state_out,
    conv_out,
):
    n = lax.axis_size("sp")
    rows, half = activations.shape
    groups, state = rotation.shape
    chans = state_proj.shape[1]
    cwide = value_proj.shape[1]
    outs = state_out.shape[1]
    states = groups * state
    prow = states // LANES
    bdw = 2 * states // (chans // LANES)
    vmem = pl.BlockSpec(memory_space=pltpu.VMEM)
    hbm = pl.BlockSpec(memory_space=pl.ANY)
    dma = pltpu.SemaphoreType.DMA
    return pl.pallas_call(
        functools.partial(kernel, n),
        out_shape=jax.ShapeDtypeStruct((rows, outs), BF16),
        in_specs=[vmem, vmem, hbm, hbm, hbm, hbm] + [vmem] * 7 + [hbm, hbm],
        out_specs=vmem,
        scratch_shapes=[
            pltpu.VMEM((4, 2, half, chans), BF16),
            pltpu.VMEM((2, 2, chans, outs), BF16),
            pltpu.VMEM((rows, half), BF16),
            pltpu.VMEM((4, rows, chans), F32),
            pltpu.VMEM((rows, chans), BF16),
            pltpu.VMEM((chans, bdw), BF16),
            pltpu.VMEM((chans, bdw), BF16),
            pltpu.VMEM((rows, states), F32),
            pltpu.VMEM((rows * prow, LANES), F32),
            pltpu.VMEM((rows * 2 * prow, LANES), F32),
            pltpu.VMEM((3 * groups, LANES), F32),
            pltpu.VMEM((rows + 8, cwide), F32),
            pltpu.VMEM((3 * prow, LANES), F32),
            pltpu.VMEM((n, 3 * prow, LANES), F32),
            pltpu.VMEM((2, rows, chans), BF16),
            pltpu.VMEM((2, rows, cwide), BF16),
            pltpu.VMEM((rows, outs), F32),
            dma((4, 2)),
            dma((2, 2)),
            dma((2,)),
            dma((2,)),
            dma((2,)),
            dma((2, chans // (2 * LANES))),
            dma((n,)),
            dma((n,)),
        ],
        compiler_params=pltpu.CompilerParams(collective_id=0, has_side_effects=True),
    )(
        activations,
        norm_gain.reshape(1, -1),
        state_proj,
        value_proj,
        post_gate_proj,
        pre_gate_proj,
        input_map,
        jnp.swapaxes(output_map, 1, 2),
        skip_gain.reshape(1, -1),
        rotation,
        jnp.swapaxes(log_decay, 0, 1),
        initial_state,
        conv_taps,
        state_out,
        conv_out,
    )


def solution(mesh):
    return jax.shard_map(
        on_device,
        mesh=mesh,
        in_specs=(
            P("sp", "tp"),
            P(),
            P(None, "tp"),
            P(None, "tp"),
            P(None, "tp"),
            P(None, "tp"),
            P("tp", None, None),
            P("tp", None, None),
            P("tp"),
            P("tp", None),
            P("sp", "tp"),
            P(None, "tp", None),
            P(None, "tp"),
            P(None, "tp"),
            P(None, "tp"),
        ),
        out_specs=P("sp", "tp"),
        check_vma=False,
    )
```

```python
import functools

import jax
import jax.numpy as jnp
from jax import lax
from jax.experimental import pallas as pl
from jax.experimental.pallas import tpu as pltpu
from jax.sharding import PartitionSpec as P

EPS = 1e-06
LANES = 128
MESH = pl.DeviceIdType.MESH
F32 = jnp.float32
BF16 = jnp.bfloat16


def minus_expm1(y):
    poly = jnp.ones_like(y)
    for k in range(11, 1, -1):
        poly = 1.0 + poly * y * (1.0 / k)
    return jnp.where(y > -0.5, -y * poly, 1.0 - jnp.exp(y))


def split3(v):
    hi = v.astype(BF16)
    rest = v - hi.astype(F32)
    mid = rest.astype(BF16)
    low = (rest - mid.astype(F32)).astype(BF16)
    return hi, mid, low


def cmul(a, b):
    return a[0] * b[0] - a[1] * b[1], a[0] * b[1] + a[1] * b[0]


def cpow(base, count):
    result = None
    while count:
        if count & 1:
            result = base if result is None else cmul(result, base)
        count >>= 1
        if count:
            base = cmul(base, base)
    return result


def gelu(x):
    return 0.5 * x * (1.0 + jnp.tanh(0.7978845608028654 * (x + 0.044715 * x * x * x)))


def kernel(
    n,
    x_hbm,
    gain_hbm,
    w0_hbm,
    w1_hbm,
    w2_hbm,
    w3_hbm,
    imap_hbm,
    omap_hbm,
    skip_hbm,
    rot_hbm,
    ld_hbm,
    init_hbm,
    taps_hbm,
    so_hbm,
    co_hbm,
    out_ref,
    x_ref,
    gain_ref,
    imap_ref,
    omap_ref,
    skip_ref,
    rot_ref,
    ld_ref,
    init_ref,
    taps_ref,
    wv,
    ov,
    xr,
    acc,
    din,
    bd_in,
    bd_out,
    wide_w,
    mag,
    drv,
    pairs,
    pad,
    pay,
    ends,
    tot,
    tots,
    hs,
    hc,
    oacc,
    in_sem,
    wsem,
    osem,
    x_sem,
    tail_sem,
    hc_sem,
    hs_sem,
    send_sem,
    recv_sem,
    tsend_sem,
    trecv_sem,
):
    sp, tp = lax.axis_index("sp"), lax.axis_index("tp")
    other = 1 - tp
    rows, half = x_ref.shape
    groups, state = rot_ref.shape
    gch = imap_ref.shape[1]
    chans = groups * gch
    states = groups * state
    prow = states // LANES
    per_block = LANES // gch
    blocks = groups // per_block
    quads = prow // blocks
    pitch = drv.shape[0] // rows
    bstates = quads * LANES
    cwide = taps_ref.shape[1]
    width = taps_ref.shape[0]

    barrier = pltpu.get_barrier_semaphore()

    def greet(j, c):
        pl.semaphore_signal(
            barrier, inc=1, device_id={"sp": lax.rem(sp + j, n), "tp": tp}, device_id_type=MESH
        )
        return c

    pl.semaphore_signal(barrier, inc=1, device_id={"sp": sp, "tp": other}, device_id_type=MESH)
    lax.fori_loop(1, n, greet, 0)

    small = []
    for i, (src, dst) in enumerate((
        (rot_hbm, rot_ref),
        (init_hbm, init_ref),
        (ld_hbm, ld_ref),
        (imap_hbm, imap_ref),
        (omap_hbm, omap_ref),
        (x_hbm, x_ref),
        (gain_hbm, gain_ref),
        (skip_hbm, skip_ref),
        (taps_hbm, taps_ref),
    )):
        copy = pltpu.make_async_copy(src, dst, in_sem.at[i])
        copy.start()
        small.append(copy)

    wcopies = {}
    for h, part in ((0, tp), (1, other)):
        for i, w in enumerate((w0_hbm, w1_hbm, w2_hbm, w3_hbm)):
            copy = pltpu.make_async_copy(
                w.at[pl.ds(part * half, half), :], wv.at[i, h], wsem.at[i, h]
            )
            copy.start()
            wcopies[i, h] = copy
    ocopies = {}
    for i, w, deep in ((1, co_hbm, cwide), (0, so_hbm, chans)):
        for h, part in ((0, tp), (1, other)):
            copy = pltpu.make_async_copy(w.at[pl.ds(part * deep, deep), :], ov.at[i, h], osem.at[i, h])
            copy.start()
            ocopies[i, h] = copy

    for copy in small:
        copy.wait()

    lane = lax.broadcasted_iota(jnp.int32, (1, LANES), 1)
    for i, v in enumerate((rot_ref[...], init_ref[0], init_ref[1])):
        pairs[pl.ds(i * groups, groups), :] = jnp.concatenate([v, v], axis=1)

    def paired(i):
        even = pairs[pl.ds(i * groups, prow, stride=2), :]
        odd = pairs[pl.ds(i * groups + 1, prow, stride=2), :]
        return jnp.where(lane < state, even, odd)

    theta = paired(0)
    cosv, sinv = jnp.cos(theta), jnp.sin(theta)
    whole = cpow((cosv, sinv), rows)

    for src, dst in ((imap_ref, bd_in), (omap_ref, bd_out)):
        dst[...] = jnp.zeros_like(dst)
        for b in range(blocks):
            for q in range(quads):
                g = b * per_block + 2 * q
                one = src[g].astype(F32)
                two = src[g + 1].astype(F32)
                one_r = jnp.concatenate([one[:, state:], one[:, :state]], axis=1)
                two_r = jnp.concatenate([two[:, state:], two[:, :state]], axis=1)
                low = lane < state
                re = jnp.concatenate([jnp.where(low, one, 0.0), jnp.where(low, 0.0, two_r)], axis=0)
                im = jnp.concatenate([jnp.where(low, one_r, 0.0), jnp.where(low, 0.0, two)], axis=0)
                at = pl.ds(b * LANES + q * 2 * gch, 2 * gch)
                dst[at, q * LANES : (q + 1) * LANES] = re.astype(BF16)
                dst[at, bstates + q * LANES : bstates + (q + 1) * LANES] = im.astype(BF16)

    ld = ld_ref[...].T
    mags = split3(jnp.exp(ld))
    whole_mags = split3(jnp.exp(jnp.sum(ld, axis=0, keepdims=True)))
    gains = split3(jnp.sqrt(minus_expm1(2.0 * ld)))[:2]
    for b in range(blocks):
        col = lax.broadcasted_iota(jnp.int32, (groups, bstates), 1) + b * bstates
        row = lax.broadcasted_iota(jnp.int32, (groups, bstates), 0)
        spread = jnp.where(
            (col >= row * state) & (col < (row + 1) * state), 1.0, 0.0
        ).astype(BF16)

        def over(pieces):
            total = None
            for piece in pieces:
                d = jnp.dot(piece, spread, preferred_element_type=F32)
                total = d if total is None else total + d
            return total

        m = over(mags)
        for q in range(quads):
            mag[pl.ds(b * quads + q, rows, stride=prow), :] = m[:, q * LANES : (q + 1) * LANES]
        m = over(whole_mags)
        for q in range(quads):
            tot[b * quads + q : b * quads + q + 1, :] = m[:, q * LANES : (q + 1) * LANES]
        wide_w[:, b * bstates : (b + 1) * bstates] = over(gains)

    pl.semaphore_wait(barrier, n)
    partner = {"sp": sp, "tp": other}

    def remote(src, dst, s, r, dev):
        return pltpu.make_async_remote_copy(
            src_ref=src, dst_ref=dst, send_sem=s, recv_sem=r, device_id=dev, device_id_type=MESH
        )

    x_copy = remote(x_ref, xr, x_sem.at[0], x_sem.at[1], partner)
    x_copy.start()

    def tot_copy(j):
        return remote(
            tot, tots.at[sp], tsend_sem.at[j], trecv_sem.at[sp], {"sp": j, "tp": tp}
        )

    def send_tot(j, c):
        tot_copy(j).start()
        return c

    lax.fori_loop(sp + 1, n, send_tot, 0)

    own = x_ref[...].astype(F32)
    scaled = (own * gain_ref[:, pl.ds(pl.multiple_of(tp * half, LANES), half)]).astype(BF16)
    squares = jnp.sum(own * own, axis=1, keepdims=True)
    for i in range(4):
        wcopies[i, 0].wait()
        acc[i] = jnp.dot(scaled, wv[i, 0], preferred_element_type=F32)

    x_copy.wait_recv()
    far = xr[...].astype(F32)
    scaled_far = (far * gain_ref[:, pl.ds(pl.multiple_of(other * half, LANES), half)]).astype(BF16)
    squares = squares + jnp.sum(far * far, axis=1, keepdims=True)
    scale = lax.rsqrt(squares / (2 * half) + EPS)

    def project(i):
        wcopies[i, 1].wait()
        total = acc[i] + jnp.dot(scaled_far, wv[i, 1], preferred_element_type=F32)
        return (total * scale).astype(BF16)

    drive_in = project(0)
    din[...] = drive_in
    for b in range(blocks):
        blk = jnp.dot(
            drive_in[:, b * LANES : (b + 1) * LANES],
            bd_in[b * LANES : (b + 1) * LANES, :],
            preferred_element_type=F32,
        )
        for q in range(quads):
            r = b * quads + q
            w = wide_w[:, r * LANES : (r + 1) * LANES]
            drv[pl.ds(r, rows, stride=pitch), :] = blk[:, q * LANES : (q + 1) * LANES] * w
            drv[pl.ds(prow + r, rows, stride=pitch), :] = (
                blk[:, bstates + q * LANES : bstates + (q + 1) * LANES] * w
            )

    def advance(t, h):
        m = mag[pl.ds(pl.multiple_of(t * prow, prow), prow), :]
        base = pl.multiple_of(t * pitch, 8)
        d_re = drv[pl.ds(base, prow), :]
        d_im = drv[pl.ds(base + prow, prow), :]
        f_re, f_im = m * cosv, m * sinv
        new_re = (f_re * h[0] + d_re) - f_im * h[1]
        new_im = (f_re * h[1] + d_im) + f_im * h[0]
        return base, (new_re, new_im)

    def first(t, c):
        base, h = advance(t, c)
        return h

    zero = jnp.zeros((prow, LANES), F32)
    e_re, e_im = lax.fori_loop(0, rows, first, (zero, zero), unroll=8)
    pay[pl.ds(0, prow), :] = e_re.astype(BF16)
    pay[pl.ds(prow, prow), :] = e_im.astype(BF16)

    def end_copy(j):
        return remote(
            pay, ends.at[sp], send_sem.at[j], recv_sem.at[sp], {"sp": j, "tp": tp}
        )

    def send_end(j, c):
        end_copy(j).start()
        return c

    lax.fori_loop(sp + 1, n, send_end, 0)

    value = project(1)
    pre_gate = project(3)
    mixed = (pre_gate.astype(F32) * value.astype(F32)).astype(BF16).astype(F32)
    pad[pl.ds(8, rows), :] = mixed
    tail_copy = remote(
        pad.at[pl.ds(rows, 8), :],
        pad.at[pl.ds(0, 8), :],
        tail_sem.at[0],
        tail_sem.at[1],
        {"sp": lax.rem(sp + 1, n), "tp": tp},
    )

    @pl.when(sp < n - 1)
    def _():
        tail_copy.start()

    post_gate = project(2).astype(F32)

    @pl.when(sp == 0)
    def _():
        pad[pl.ds(0, 8), :] = jnp.zeros((8, cwide), F32)

    @pl.when(sp > 0)
    def _():
        tail_copy.wait_recv()

    conv = jnp.zeros((rows, cwide), F32)
    for k in range(width):
        conv = conv + pad[pl.ds(8 + k - (width - 1), rows), :] * taps_ref[k : k + 1, :].astype(F32)
    hc[0] = (post_gate * conv).astype(BF16)
    hc_copy = remote(hc.at[0], hc.at[1], hc_sem.at[0], hc_sem.at[1], partner)
    hc_copy.start()
    ocopies[1, 0].wait()
    ocopies[1, 1].wait()
    oacc[...] = jnp.dot(hc[0], ov[1, 0], preferred_element_type=F32)
    hc_copy.wait_recv()
    oacc[...] += jnp.dot(hc[1], ov[1, 1], preferred_element_type=F32)

    def gather(k, h):
        remote(pay, ends.at[k], send_sem.at[k], recv_sem.at[k], {"sp": k, "tp": tp}).wait_recv()
        remote(tot, tots.at[k], tsend_sem.at[k], trecv_sem.at[k], {"sp": k, "tp": tp}).wait_recv()
        k_mag = tots[k]
        moved = cmul((whole[0] * k_mag, whole[1] * k_mag), h)
        k_re = ends[k, pl.ds(0, prow), :].astype(F32)
        k_im = ends[k, pl.ds(prow, prow), :].astype(F32)
        return moved[0] + k_re, moved[1] + k_im

    enter = lax.fori_loop(0, sp, gather, (paired(1), paired(2)))

    def second(t, c):
        base, h = advance(t, c)
        drv[pl.ds(base, prow), :] = h[0]
        drv[pl.ds(base + prow, prow), :] = h[1]
        return h

    lax.fori_loop(0, rows, second, enter, unroll=8)

    hs_copies = []
    for b in range(blocks):
        at = [b * quads + q for q in range(quads)]
        at = at + [prow + r for r in at]
        cols = slice(b * LANES, (b + 1) * LANES)
        st = jnp.concatenate(
            [drv[pl.ds(r, rows, stride=pitch), :].astype(BF16) for r in at], axis=1
        )
        read = lax.dot_general(
            st, bd_out[cols, :], (((1,), (1,)), ((), ())), preferred_element_type=F32
        )
        hs[0, :, cols] = gelu(read + skip_ref[:, cols] * din[:, cols].astype(F32)).astype(BF16)
        if b % 2 == 1:
            two = pl.ds((b - 1) * LANES, 2 * LANES)
            copy = remote(
                hs.at[0, :, two], hs.at[1, :, two], hs_sem.at[0, b // 2], hs_sem.at[1, b // 2], partner
            )
            copy.start()
            hs_copies.append(copy)
    ocopies[0, 0].wait()
    ocopies[0, 1].wait()
    oacc[...] += jnp.dot(hs[0], ov[0, 0], preferred_element_type=F32)
    for copy in hs_copies:
        copy.wait_recv()
    out_ref[...] = (oacc[...] + jnp.dot(hs[1], ov[0, 1], preferred_element_type=F32)).astype(BF16)

    x_copy.wait_send()
    hc_copy.wait_send()
    for copy in hs_copies:
        copy.wait_send()

    @pl.when(sp < n - 1)
    def _():
        tail_copy.wait_send()

    def sent(j, c):
        end_copy(j).wait_send()
        tot_copy(j).wait_send()
        return c

    lax.fori_loop(sp + 1, n, sent, 0)


def on_device(
    activations,
    norm_gain,
    state_proj,
    value_proj,
    post_gate_proj,
    pre_gate_proj,
    input_map,
    output_map,
    skip_gain,
    rotation,
    log_decay,
    initial_state,
    conv_taps,
    state_out,
    conv_out,
):
    n = lax.axis_size("sp")
    rows, half = activations.shape
    groups, state = rotation.shape
    chans = state_proj.shape[1]
    cwide = value_proj.shape[1]
    outs = state_out.shape[1]
    states = groups * state
    prow = states // LANES
    bdw = 2 * states // (chans // LANES)
    vmem = pl.BlockSpec(memory_space=pltpu.VMEM)
    hbm = pl.BlockSpec(memory_space=pl.ANY)
    dma = pltpu.SemaphoreType.DMA
    return pl.pallas_call(
        functools.partial(kernel, n),
        out_shape=pltpu.VMEM((rows, outs), BF16),
        in_specs=[hbm] * 15,
        out_specs=vmem,
        scratch_shapes=[
            pltpu.VMEM((rows, half), BF16),
            pltpu.VMEM((1, 2 * half), F32),
            pltpu.VMEM(input_map.shape, BF16),
            pltpu.VMEM((groups, output_map.shape[2], output_map.shape[1]), F32),
            pltpu.VMEM((1, chans), F32),
            pltpu.VMEM((groups, state), F32),
            pltpu.VMEM((groups, rows), F32),
            pltpu.VMEM(initial_state.shape, F32),
            pltpu.VMEM(conv_taps.shape, BF16),
            pltpu.VMEM((4, 2, half, chans), BF16),
            pltpu.VMEM((2, 2, chans, outs), BF16),
            pltpu.VMEM((rows, half), BF16),
            pltpu.VMEM((4, rows, chans), F32),
            pltpu.VMEM((rows, chans), BF16),
            pltpu.VMEM((chans, bdw), BF16),
            pltpu.VMEM((chans, bdw), BF16),
            pltpu.VMEM((rows, states), F32),
            pltpu.VMEM((rows * prow, LANES), F32),
            pltpu.VMEM((rows * (2 * prow + 8), LANES), F32),
            pltpu.VMEM((3 * groups, LANES), F32),
            pltpu.VMEM((rows + 8, cwide), F32),
            pltpu.VMEM((2 * prow, LANES), BF16),
            pltpu.VMEM((n, 2 * prow, LANES), BF16),
            pltpu.VMEM((prow, LANES), F32),
            pltpu.VMEM((n, prow, LANES), F32),
            pltpu.VMEM((2, rows, chans), BF16),
            pltpu.VMEM((2, rows, cwide), BF16),
            pltpu.VMEM((rows, outs), F32),
            dma((9,)),
            dma((4, 2)),
            dma((2, 2)),
            dma((2,)),
            dma((2,)),
            dma((2,)),
            dma((2, chans // (2 * LANES))),
            dma((n,)),
            dma((n,)),
            dma((n,)),
            dma((n,)),
        ],
        compiler_params=pltpu.CompilerParams(collective_id=0, has_side_effects=True),
    )(
        activations,
        norm_gain.reshape(1, -1),
        state_proj,
        value_proj,
        post_gate_proj,
        pre_gate_proj,
        input_map,
        jnp.swapaxes(output_map, 1, 2),
        skip_gain.reshape(1, -1),
        rotation,
        jnp.swapaxes(log_decay, 0, 1),
        initial_state,
        conv_taps,
        state_out,
        conv_out,
    )


def solution(mesh):
    return jax.shard_map(
        on_device,
        mesh=mesh,
        in_specs=(
            P("sp", "tp"),
            P(),
            P(None, "tp"),
            P(None, "tp"),
            P(None, "tp"),
            P(None, "tp"),
            P("tp", None, None),
            P("tp", None, None),
            P("tp"),
            P("tp", None),
            P("sp", "tp"),
            P(None, "tp", None),
            P(None, "tp"),
            P(None, "tp"),
            P(None, "tp"),
        ),
        out_specs=P("sp", "tp"),
        check_vma=False,
    )
```

```python
import functools

import jax
import jax.numpy as jnp
from jax import lax
from jax.experimental import pallas as pl
from jax.experimental.pallas import tpu as pltpu
from jax.sharding import PartitionSpec as P

EPS = 1e-06
LANES = 128
MESH = pl.DeviceIdType.MESH
F32 = jnp.float32
BF16 = jnp.bfloat16


def minus_expm1(y):
    poly = jnp.ones_like(y)
    for k in range(11, 1, -1):
        poly = 1.0 + poly * y * (1.0 / k)
    return jnp.where(y > -0.5, -y * poly, 1.0 - jnp.exp(y))


def split3(v):
    hi = v.astype(BF16)
    rest = v - hi.astype(F32)
    mid = rest.astype(BF16)
    low = (rest - mid.astype(F32)).astype(BF16)
    return hi, mid, low


def cmul(a, b):
    return a[0] * b[0] - a[1] * b[1], a[0] * b[1] + a[1] * b[0]


def cpow(base, count):
    result = None
    while count:
        if count & 1:
            result = base if result is None else cmul(result, base)
        count >>= 1
        if count:
            base = cmul(base, base)
    return result


def gelu(x):
    return 0.5 * x * (1.0 + jnp.tanh(0.7978845608028654 * (x + 0.044715 * x * x * x)))


def kernel(
    n,
    x_hbm,
    gain_hbm,
    w0_hbm,
    w1_hbm,
    w2_hbm,
    w3_hbm,
    imap_hbm,
    omap_hbm,
    skip_hbm,
    rot_hbm,
    ld_hbm,
    init_hbm,
    taps_hbm,
    so_hbm,
    co_hbm,
    out_ref,
    x_ref,
    gain_ref,
    imap_ref,
    omap_ref,
    skip_ref,
    rot_ref,
    ld_ref,
    init_ref,
    taps_ref,
    wv,
    ov,
    xr,
    acc,
    din,
    bd_in,
    bd_out,
    wide_w,
    mag,
    drv,
    pairs,
    pad,
    pay,
    ends,
    tot,
    tots,
    hs,
    hc,
    oacc,
    in_sem,
    wsem,
    osem,
    x_sem,
    tail_sem,
    hc_sem,
    hs_sem,
    send_sem,
    recv_sem,
    tsend_sem,
    trecv_sem,
):
    sp, tp = lax.axis_index("sp"), lax.axis_index("tp")
    other = 1 - tp
    rows, half = x_ref.shape
    groups, state = rot_ref.shape
    gch = imap_ref.shape[1]
    chans = groups * gch
    states = groups * state
    prow = states // LANES
    per_block = LANES // gch
    blocks = groups // per_block
    quads = prow // blocks
    pitch = drv.shape[0] // rows
    bstates = quads * LANES
    cwide = taps_ref.shape[1]
    width = taps_ref.shape[0]

    barrier = pltpu.get_barrier_semaphore()

    def greet(j, c):
        pl.semaphore_signal(
            barrier, inc=1, device_id={"sp": lax.rem(sp + j, n), "tp": tp}, device_id_type=MESH
        )
        return c

    pl.semaphore_signal(barrier, inc=1, device_id={"sp": sp, "tp": other}, device_id_type=MESH)
    lax.fori_loop(1, n, greet, 0)

    in_copies = {}
    def fetch(i, src, dst):
        in_copies[i] = pltpu.make_async_copy(src, dst, in_sem.at[i])
        in_copies[i].start()

    wcopies = {}

    def fetch_weight(i, h):
        w = (w0_hbm, w1_hbm, w2_hbm, w3_hbm)[i]
        part = (tp, other)[h]
        wcopies[i, h] = pltpu.make_async_copy(
            w.at[pl.ds(part * half, half), :], wv.at[i, h], wsem.at[i, h]
        )
        wcopies[i, h].start()

    fetch(0, x_hbm, x_ref)
    fetch(1, gain_hbm, gain_ref)
    fetch(2, rot_hbm, rot_ref)
    fetch(3, init_hbm, init_ref)
    fetch(4, ld_hbm, ld_ref)
    fetch(5, imap_hbm, imap_ref)
    fetch_weight(0, 0)
    fetch_weight(0, 1)
    fetch(6, omap_hbm, omap_ref)
    fetch(7, skip_hbm, skip_ref)
    fetch(8, taps_hbm, taps_ref)
    for i in (1, 3, 2):
        fetch_weight(i, 0)
        fetch_weight(i, 1)
    ocopies = {}
    for i, w, deep in ((1, co_hbm, cwide), (0, so_hbm, chans)):
        for h, part in ((0, tp), (1, other)):
            copy = pltpu.make_async_copy(w.at[pl.ds(part * deep, deep), :], ov.at[i, h], osem.at[i, h])
            copy.start()
            ocopies[i, h] = copy

    pl.semaphore_wait(barrier, n)
    partner = {"sp": sp, "tp": other}

    def remote(src, dst, s, r, dev):
        return pltpu.make_async_remote_copy(
            src_ref=src, dst_ref=dst, send_sem=s, recv_sem=r, device_id=dev, device_id_type=MESH
        )

    in_copies[0].wait()
    x_copy = remote(x_ref, xr, x_sem.at[0], x_sem.at[1], partner)
    x_copy.start()

    for i in range(2, 6):
        in_copies[i].wait()

    lane = lax.broadcasted_iota(jnp.int32, (1, LANES), 1)
    for i, v in enumerate((rot_ref[...], init_ref[0], init_ref[1])):
        pairs[pl.ds(i * groups, groups), :] = jnp.concatenate([v, v], axis=1)

    def paired(i):
        even = pairs[pl.ds(i * groups, prow, stride=2), :]
        odd = pairs[pl.ds(i * groups + 1, prow, stride=2), :]
        return jnp.where(lane < state, even, odd)

    theta = paired(0)
    cosv, sinv = jnp.cos(theta), jnp.sin(theta)
    whole = cpow((cosv, sinv), rows)

    def spread_map(src, dst):
        dst[...] = jnp.zeros_like(dst)
        for b in range(blocks):
            for q in range(quads):
                g = b * per_block + 2 * q
                one = src[g].astype(F32)
                two = src[g + 1].astype(F32)
                one_r = jnp.concatenate([one[:, state:], one[:, :state]], axis=1)
                two_r = jnp.concatenate([two[:, state:], two[:, :state]], axis=1)
                low = lane < state
                re = jnp.concatenate([jnp.where(low, one, 0.0), jnp.where(low, 0.0, two_r)], axis=0)
                im = jnp.concatenate([jnp.where(low, one_r, 0.0), jnp.where(low, 0.0, two)], axis=0)
                at = pl.ds(b * LANES + q * 2 * gch, 2 * gch)
                dst[at, q * LANES : (q + 1) * LANES] = re.astype(BF16)
                dst[at, bstates + q * LANES : bstates + (q + 1) * LANES] = im.astype(BF16)

    spread_map(imap_ref, bd_in)

    ld = ld_ref[...].T
    mags = split3(jnp.exp(ld))
    whole_mags = split3(jnp.exp(jnp.sum(ld, axis=0, keepdims=True)))
    gains = split3(jnp.sqrt(minus_expm1(2.0 * ld)))[:2]
    for b in range(blocks):
        col = lax.broadcasted_iota(jnp.int32, (groups, bstates), 1) + b * bstates
        row = lax.broadcasted_iota(jnp.int32, (groups, bstates), 0)
        spread = jnp.where(
            (col >= row * state) & (col < (row + 1) * state), 1.0, 0.0
        ).astype(BF16)

        def over(pieces):
            total = None
            for piece in pieces:
                d = jnp.dot(piece, spread, preferred_element_type=F32)
                total = d if total is None else total + d
            return total

        m = over(mags)
        for q in range(quads):
            mag[pl.ds(b * quads + q, rows, stride=prow), :] = m[:, q * LANES : (q + 1) * LANES]
        m = over(whole_mags)
        for q in range(quads):
            tot[b * quads + q : b * quads + q + 1, :] = m[:, q * LANES : (q + 1) * LANES]
        wide_w[:, b * bstates : (b + 1) * bstates] = over(gains)

    def tot_copy(j):
        return remote(
            tot, tots.at[sp], tsend_sem.at[j], trecv_sem.at[sp], {"sp": j, "tp": tp}
        )

    def send_tot(j, c):
        tot_copy(j).start()
        return c

    lax.fori_loop(sp + 1, n, send_tot, 0)

    in_copies[1].wait()
    own = x_ref[...].astype(F32)
    scaled = (own * gain_ref[:, pl.ds(pl.multiple_of(tp * half, LANES), half)]).astype(BF16)
    squares = jnp.sum(own * own, axis=1, keepdims=True)
    wcopies[0, 0].wait()
    partial = jnp.dot(scaled, wv[0, 0], preferred_element_type=F32)
    acc[0] = scaled

    x_copy.wait_recv()
    far = xr[...].astype(F32)
    scaled_far = (far * gain_ref[:, pl.ds(pl.multiple_of(other * half, LANES), half)]).astype(BF16)
    squares = squares + jnp.sum(far * far, axis=1, keepdims=True)
    scale = lax.rsqrt(squares / (2 * half) + EPS)

    acc[1] = scaled_far
    wcopies[0, 1].wait()
    total = partial + jnp.dot(scaled_far, wv[0, 1], preferred_element_type=F32)
    drive_in = (total * scale).astype(BF16)
    din[...] = drive_in
    for b in range(blocks):
        blk = jnp.dot(
            drive_in[:, b * LANES : (b + 1) * LANES],
            bd_in[b * LANES : (b + 1) * LANES, :],
            preferred_element_type=F32,
        )
        for q in range(quads):
            r = b * quads + q
            w = wide_w[:, r * LANES : (r + 1) * LANES]
            drv[pl.ds(r, rows, stride=pitch), :] = blk[:, q * LANES : (q + 1) * LANES] * w
            drv[pl.ds(prow + r, rows, stride=pitch), :] = (
                blk[:, bstates + q * LANES : bstates + (q + 1) * LANES] * w
            )

    def advance(t, h):
        m = mag[pl.ds(pl.multiple_of(t * prow, prow), prow), :]
        base = pl.multiple_of(t * pitch, 8)
        d_re = drv[pl.ds(base, prow), :]
        d_im = drv[pl.ds(base + prow, prow), :]
        f_re, f_im = m * cosv, m * sinv
        new_re = (f_re * h[0] + d_re) - f_im * h[1]
        new_im = (f_re * h[1] + d_im) + f_im * h[0]
        return base, (new_re, new_im)

    def first(t, c):
        base, h = advance(t, c)
        return h

    zero = jnp.zeros((prow, LANES), F32)
    e_re, e_im = lax.fori_loop(0, rows, first, (zero, zero), unroll=8)
    pay[pl.ds(0, prow), :] = e_re.astype(BF16)
    pay[pl.ds(prow, prow), :] = e_im.astype(BF16)

    def end_copy(j):
        return remote(
            pay, ends.at[sp], send_sem.at[j], recv_sem.at[sp], {"sp": j, "tp": tp}
        )

    def send_end(j, c):
        end_copy(j).start()
        return c

    lax.fori_loop(sp + 1, n, send_end, 0)

    def project(i):
        wcopies[i, 0].wait()
        wcopies[i, 1].wait()
        total = jnp.dot(acc[0], wv[i, 0], preferred_element_type=F32)
        total = total + jnp.dot(acc[1], wv[i, 1], preferred_element_type=F32)
        return (total * scale).astype(BF16)

    value = project(1)
    pre_gate = project(3)
    mixed = (pre_gate.astype(F32) * value.astype(F32)).astype(BF16).astype(F32)
    pad[pl.ds(8, rows), :] = mixed
    tail_copy = remote(
        pad.at[pl.ds(rows, 8), :],
        pad.at[pl.ds(0, 8), :],
        tail_sem.at[0],
        tail_sem.at[1],
        {"sp": lax.rem(sp + 1, n), "tp": tp},
    )

    @pl.when(sp < n - 1)
    def _():
        tail_copy.start()

    hc[0] = project(2)

    for i in (6, 7):
        in_copies[i].wait()
    spread_map(omap_ref, bd_out)

    def gather(k, h):
        remote(pay, ends.at[k], send_sem.at[k], recv_sem.at[k], {"sp": k, "tp": tp}).wait_recv()
        remote(tot, tots.at[k], tsend_sem.at[k], trecv_sem.at[k], {"sp": k, "tp": tp}).wait_recv()
        k_mag = tots[k]
        moved = cmul((whole[0] * k_mag, whole[1] * k_mag), h)
        k_re = ends[k, pl.ds(0, prow), :].astype(F32)
        k_im = ends[k, pl.ds(prow, prow), :].astype(F32)
        return moved[0] + k_re, moved[1] + k_im

    enter = lax.fori_loop(0, sp, gather, (paired(1), paired(2)))

    def second(t, c):
        base, h = advance(t, c)
        drv[pl.ds(base, prow), :] = h[0]
        drv[pl.ds(base + prow, prow), :] = h[1]
        return h

    lax.fori_loop(0, rows, second, enter, unroll=8)

    @pl.when(sp == 0)
    def _():
        pad[pl.ds(0, 8), :] = jnp.zeros((8, cwide), F32)

    in_copies[8].wait()

    @pl.when(sp > 0)
    def _():
        tail_copy.wait_recv()

    conv = jnp.zeros((rows, cwide), F32)
    for k in range(width):
        conv = conv + pad[pl.ds(8 + k - (width - 1), rows), :] * taps_ref[k : k + 1, :].astype(F32)
    hc[0] = (hc[0].astype(F32) * conv).astype(BF16)
    hc_copy = remote(hc.at[0], hc.at[1], hc_sem.at[0], hc_sem.at[1], partner)
    hc_copy.start()
    hs_copies = []
    for b in range(blocks):
        at = [b * quads + q for q in range(quads)]
        at = at + [prow + r for r in at]
        cols = slice(b * LANES, (b + 1) * LANES)
        st = jnp.concatenate(
            [drv[pl.ds(r, rows, stride=pitch), :].astype(BF16) for r in at], axis=1
        )
        read = lax.dot_general(
            st, bd_out[cols, :], (((1,), (1,)), ((), ())), preferred_element_type=F32
        )
        hs[0, :, cols] = gelu(read + skip_ref[:, cols] * din[:, cols].astype(F32)).astype(BF16)
        if b % 2 == 1:
            two = pl.ds((b - 1) * LANES, 2 * LANES)
            copy = remote(
                hs.at[0, :, two], hs.at[1, :, two], hs_sem.at[0, b // 2], hs_sem.at[1, b // 2], partner
            )
            copy.start()
            hs_copies.append(copy)
    for i in (0, 1):
        for h in (0, 1):
            ocopies[i, h].wait()
    oacc[...] = jnp.dot(hc[0], ov[1, 0], preferred_element_type=F32)
    oacc[...] += jnp.dot(hs[0], ov[0, 0], preferred_element_type=F32)
    hc_copy.wait_recv()
    oacc[...] += jnp.dot(hc[1], ov[1, 1], preferred_element_type=F32)
    for copy in hs_copies:
        copy.wait_recv()
    out_ref[...] = (oacc[...] + jnp.dot(hs[1], ov[0, 1], preferred_element_type=F32)).astype(BF16)

    x_copy.wait_send()
    hc_copy.wait_send()
    for copy in hs_copies:
        copy.wait_send()

    @pl.when(sp < n - 1)
    def _():
        tail_copy.wait_send()

    def sent(j, c):
        end_copy(j).wait_send()
        tot_copy(j).wait_send()
        return c

    lax.fori_loop(sp + 1, n, sent, 0)


def on_device(
    activations,
    norm_gain,
    state_proj,
    value_proj,
    post_gate_proj,
    pre_gate_proj,
    input_map,
    output_map,
    skip_gain,
    rotation,
    log_decay,
    initial_state,
    conv_taps,
    state_out,
    conv_out,
):
    n = lax.axis_size("sp")
    rows, half = activations.shape
    groups, state = rotation.shape
    chans = state_proj.shape[1]
    cwide = value_proj.shape[1]
    outs = state_out.shape[1]
    states = groups * state
    prow = states // LANES
    bdw = 2 * states // (chans // LANES)
    vmem = pl.BlockSpec(memory_space=pltpu.VMEM)
    hbm = pl.BlockSpec(memory_space=pl.ANY)
    dma = pltpu.SemaphoreType.DMA
    return pl.pallas_call(
        functools.partial(kernel, n),
        out_shape=pltpu.VMEM((rows, outs), BF16),
        in_specs=[hbm] * 15,
        out_specs=vmem,
        scratch_shapes=[
            pltpu.VMEM((rows, half), BF16),
            pltpu.VMEM((1, 2 * half), F32),
            pltpu.VMEM(input_map.shape, BF16),
            pltpu.VMEM((groups, output_map.shape[2], output_map.shape[1]), F32),
            pltpu.VMEM((1, chans), F32),
            pltpu.VMEM((groups, state), F32),
            pltpu.VMEM((groups, rows), F32),
            pltpu.VMEM(initial_state.shape, F32),
            pltpu.VMEM(conv_taps.shape, BF16),
            pltpu.VMEM((4, 2, half, chans), BF16),
            pltpu.VMEM((2, 2, chans, outs), BF16),
            pltpu.VMEM((rows, half), BF16),
            pltpu.VMEM((2, rows, half), BF16),
            pltpu.VMEM((rows, chans), BF16),
            pltpu.VMEM((chans, bdw), BF16),
            pltpu.VMEM((chans, bdw), BF16),
            pltpu.VMEM((rows, states), F32),
            pltpu.VMEM((rows * prow, LANES), F32),
            pltpu.VMEM((rows * (2 * prow + 8), LANES), F32),
            pltpu.VMEM((3 * groups, LANES), F32),
            pltpu.VMEM((rows + 8, cwide), F32),
            pltpu.VMEM((2 * prow, LANES), BF16),
            pltpu.VMEM((n, 2 * prow, LANES), BF16),
            pltpu.VMEM((prow, LANES), F32),
            pltpu.VMEM((n, prow, LANES), F32),
            pltpu.VMEM((2, rows, chans), BF16),
            pltpu.VMEM((2, rows, cwide), BF16),
            pltpu.VMEM((rows, outs), F32),
            dma((9,)),
            dma((4, 2)),
            dma((2, 2)),
            dma((2,)),
            dma((2,)),
            dma((2,)),
            dma((2, chans // (2 * LANES))),
            dma((n,)),
            dma((n,)),
            dma((n,)),
            dma((n,)),
        ],
        compiler_params=pltpu.CompilerParams(collective_id=0, has_side_effects=True),
    )(
        activations,
        norm_gain.reshape(1, -1),
        state_proj,
        value_proj,
        post_gate_proj,
        pre_gate_proj,
        input_map,
        jnp.swapaxes(output_map, 1, 2),
        skip_gain.reshape(1, -1),
        rotation,
        jnp.swapaxes(log_decay, 0, 1),
        initial_state,
        conv_taps,
        state_out,
        conv_out,
    )


def solution(mesh):
    return jax.shard_map(
        on_device,
        mesh=mesh,
        in_specs=(
            P("sp", "tp"),
            P(),
            P(None, "tp"),
            P(None, "tp"),
            P(None, "tp"),
            P(None, "tp"),
            P("tp", None, None),
            P("tp", None, None),
            P("tp"),
            P("tp", None),
            P("sp", "tp"),
            P(None, "tp", None),
            P(None, "tp"),
            P(None, "tp"),
            P(None, "tp"),
        ),
        out_specs=P("sp", "tp"),
        check_vma=False,
    )
```
